256 devices in a mesh: sp: 32 (over z, y), tp: 8 (over x, core).
Axes of the slice: x: 4, y: 4, z: 8, core: 2. Of those that a mesh axis runs over, the one named last changes fastest.
Arguments:
- tokens: bfloat16 [32768, 2048], P('sp'), may hold values from -6 to 6
- in_gain: float32 [2048], replicated, may hold values from 0.1 to 1.9
- w_query: bfloat16 [2048, 1024], P(None, 'tp'), may hold values from -0.125 to 0.125
- w_forget: bfloat16 [2048, 1024], P(None, 'tp'), may hold values from -0.125 to 0.125
- w_input: bfloat16 [2048, 1024], P(None, 'tp'), may hold values from -0.125 to 0.125
- w_outgate: bfloat16 [2048, 1024], P(None, 'tp'), may hold values from -0.125 to 0.125
- w_conv_h: bfloat16 [2048, 1024], P(None, 'tp'), may hold values from -0.125 to 0.125
- w_conv_b: bfloat16 [2048, 1024], P(None, 'tp'), may hold values from -0.125 to 0.125
- w_conv_c: bfloat16 [2048, 1024], P(None, 'tp'), may hold values from -0.125 to 0.125
- forget_floor: float32 [1024], P('tp'), may hold values from 0.84 to 1
- forget_leak: float32 [32768, 1024], P('sp', 'tp'), may hold values from -1 to 0
- state_gain: float32 [128], replicated, may hold values from 0.1 to 1.9
- conv_taps: bfloat16 [3, 1024], P(None, 'tp'), may hold values from -3.5 to 3.5
- group_gain: float32 [128], replicated, may hold values from 0.1 to 1.9
- out_state: bfloat16 [1024, 2048], P('tp'), may hold values from -0.1875 to 0.1875
- out_conv: bfloat16 [1024, 2048], P('tp'), may hold values from -0.1875 to 0.1875
Outputs:
- mixed_out: bfloat16 [32768, 2048], P('sp', 'tp')
The draws below stay inside these ranges and needn't reach their ends.
All inputs are finite; a program needn't handle non-finite values.
Results may differ from the reference program's by a relative error of at most 0.015.
Values may be sent and summed in bfloat16 or wider, within the bound.
A program may use at most 128 MiB of HBM per device.

```python
import jax
import jax.numpy as jnp
from jax import lax

D = 2048
GROUP_FEATURES = 128
MIXER_COUNT = 8
CONV_CH = 1024
BLOCK = 64
TAPS = 3
TOK_DEV = 1024
STEP_COUNT = 32768
STATE_W = 1024
MIX = 2048


def draw_forget_floor(key, part):
    key_fast, key_gap, key_slow = jax.random.split(jax.random.fold_in(key, 11), 3)
    share = 0.5
    is_fast = jax.random.uniform(key_fast, (MIXER_COUNT,)) < share
    is_fast = jnp.repeat(is_fast, GROUP_FEATURES)
    fast_gap = jnp.exp(jax.random.uniform(key_gap, (STATE_W,), jnp.float32, jnp.log(0.05), jnp.log(0.15)))
    slow_gap = jnp.exp(jax.random.uniform(key_slow, (STATE_W,), jnp.float32, jnp.log(0.2), jnp.log(1.0))) / STEP_COUNT
    return (1.0 - jnp.where(is_fast, fast_gap, slow_gap)).astype(jnp.float32)


def draw_forget_leak(key, part):
    key_scale, random_seed_site, key_depth, key_jitter = jax.random.split(jax.random.fold_in(key, 23), 4)
    nblk = STEP_COUNT // TOK_DEV
    low, high = (jnp.log(0.5), jnp.log(2.0))
    block_scale = jnp.exp(jax.random.uniform(key_scale, (nblk, MIXER_COUNT), jnp.float32, low, high))
    block_scale = jnp.repeat(jnp.repeat(block_scale, TOK_DEV, axis=0), GROUP_FEATURES, axis=1)
    jitter = jax.random.uniform(key_jitter, (STEP_COUNT, STATE_W), jnp.float32, 0.5, 1.5)
    starting_shift = -0.2 / STEP_COUNT * block_scale * jitter
    span_start = jax.random.randint(random_seed_site, (3, MIXER_COUNT), 0, STEP_COUNT)
    layer_number = jax.random.uniform(key_depth, (3, MIXER_COUNT), jnp.float32, jnp.log(0.5), jnp.log(0.8))
    element_places = jnp.arange(STEP_COUNT)[:, None]
    span_sizes = jnp.zeros((STEP_COUNT, MIXER_COUNT), jnp.float32)
    for entry_number in range(3):
        span_sizes = span_sizes + jnp.where(element_places == span_start[entry_number][None, :], layer_number[entry_number][None, :], 0.0)
    return (starting_shift + jnp.repeat(span_sizes, GROUP_FEATURES, axis=1)).astype(jnp.float32)


def with_spikes(values, key, source, target, parts, factor):
    owner, partner = [(jnp.arange(values.shape[position]) // (values.shape[position] // parts)).reshape([-1 if axis == position else 1 for axis in range(values.ndim)]) for position in (source, target)]
    chosen = jax.random.permutation(key, parts)[partner]
    strong = (owner == chosen) | (owner == (partner + parts // 2) % parts)
    return jnp.where(strong, factor * values, values)


def levels(key, dims, pieces, least, largest):
    level, own = 1.0, jax.random.fold_in(key, 6)
    for dim, parts in pieces:
        steps = jnp.exp(jax.random.uniform(jax.random.fold_in(own, dim), (parts,), jnp.float32, least / len(pieces), largest / len(pieces)))
        level = level * jnp.repeat(steps, dims[dim] // parts).reshape([-1 if axis == dim else 1 for axis in range(len(dims))])
    return level


def centred(rng, extent, spread, reach, cuts=(), held_as=jnp.bfloat16):
    loudness = levels(rng, extent, cuts, -0.22, 0.18) if cuts else 1.0
    array = jax.random.normal(rng, extent, jnp.float32) * spread * loudness
    return jnp.minimum(jnp.maximum(array, -reach), reach).astype(held_as)


def heavy_noise(own_key, dims, width, limit, shards, heavy, dtype=jnp.bfloat16):
    values = width * jax.random.normal(own_key, dims, jnp.float32)
    if shards:
        values = values * levels(own_key, dims, shards, -0.22, 0.18)
    return jnp.clip(with_spikes(values, jax.random.fold_in(own_key, 3), *heavy), -limit, limit).astype(dtype)


def setup_inputs(seed: int = 0) -> dict:
    streams_of = jax.random.split(jax.random.key(seed), 17)
    return {
        "tokens": centred(streams_of[0], (STEP_COUNT, D), 1.0, 6.0, ((0, 32),)),
        "in_gain": jnp.clip(1.0 + 0.18 * jax.random.normal(streams_of[1], (D,), jnp.float32), 0.1, 1.9),
        "w_query": centred(streams_of[2], (D, STATE_W), D ** -0.5, 0.125, ((1, 8),)),
        "w_forget": centred(streams_of[3], (D, STATE_W), D ** -0.5, 0.125, ((1, 8),)),
        "w_input": centred(streams_of[4], (D, STATE_W), D ** -0.5, 0.125, ((1, 8),)),
        "w_outgate": centred(streams_of[5], (D, STATE_W), D ** -0.5, 0.125, ((1, 8),)),
        "w_conv_h": centred(streams_of[6], (D, CONV_CH), D ** -0.5, 0.125, ((1, 8),)),
        "w_conv_b": centred(streams_of[7], (D, CONV_CH), D ** -0.5, 0.125, ((1, 8),)),
        "w_conv_c": centred(streams_of[8], (D, CONV_CH), D ** -0.5, 0.125, ((1, 8),)),
        "forget_floor": draw_forget_floor(jax.random.fold_in(streams_of[16], 71), 0),
        "forget_leak": draw_forget_leak(jax.random.fold_in(streams_of[16], 71), 0),
        "state_gain": jnp.clip(1.0 + 0.18 * jax.random.normal(streams_of[11], (GROUP_FEATURES,), jnp.float32), 0.1, 1.9),
        "conv_taps": centred(streams_of[12], (TAPS, CONV_CH), TAPS ** -0.5, 3.5, ((1, 8),)),
        "group_gain": jnp.clip(1.0 + 0.18 * jax.random.normal(streams_of[13], (GROUP_FEATURES,), jnp.float32), 0.1, 1.9),
        "out_state": heavy_noise(streams_of[14], (STATE_W, D), MIX ** -0.5, 0.1875, ((0, 8),), (0, 1, 8, 2.0)),
        "out_conv": heavy_noise(streams_of[15], (CONV_CH, D), MIX ** -0.5, 0.1875, ((0, 8),), (0, 1, 8, 2.0)),
    }


norm_eps = 1e-06
highest = lax.Precision.HIGHEST

def rms_rows(values, gain):
    scale = lax.rsqrt(lax.optimization_barrier(jnp.mean(values * values, axis=-1, keepdims=True)) + norm_eps)
    return values * scale * gain.astype(jnp.float32)

def state_block(carry_state, inputs):
    query_blk, key_blk, value_blk, logf_blk = inputs
    cum_log = jnp.cumsum(logf_blk, axis=1)
    carried = jnp.einsum('hcd,hde->hce', query_blk * jnp.exp(cum_log), carry_state, precision=highest)
    length = logf_blk.shape[1]
    causal = (jnp.arange(length)[:, None] >= jnp.arange(length)[None, :])[None, :, :, None]
    diff_log = cum_log[:, :, None, :] - cum_log[:, None, :, :]
    decay_all = jnp.exp(jnp.where(causal, diff_log, -jnp.inf))
    scores = jnp.einsum('hid,hjd,hijd->hij', query_blk, key_blk, decay_all, precision=highest)
    result = carried + jnp.einsum('hij,hje->hie', scores, value_blk, precision=highest)
    last_log = cum_log[:, -1, :]
    fresh = jnp.einsum('hcd,hce->hde', key_blk * jnp.exp(last_log[:, None, :] - cum_log), value_blk, precision=highest)
    new_state = jnp.exp(last_log)[:, :, None] * carry_state + fresh
    return (new_state, result)

def reference(tokens, in_gain, w_query, w_forget, w_input, w_outgate, w_conv_h, w_conv_b, w_conv_c, forget_floor, forget_leak, state_gain, conv_taps, group_gain, out_state, out_conv):
    count = tokens.shape[0]
    heads = MIXER_COUNT
    normed = rms_rows(tokens.astype(jnp.float32), in_gain).astype(jnp.bfloat16)

    def project(weight):
        return jnp.dot(normed, weight, preferred_element_type=jnp.float32).astype(jnp.bfloat16)
    proj_query = project(w_query)
    proj_forget = project(w_forget)
    proj_input = project(w_input)
    proj_outgate = project(w_outgate)
    proj_h = project(w_conv_h)
    proj_b = project(w_conv_b)
    proj_c = project(w_conv_c)
    gate_logit = proj_forget.astype(jnp.float32)
    log_forget = jnp.logaddexp(jnp.log(forget_floor), jnp.log1p(-forget_floor) + jax.nn.log_sigmoid(gate_logit)) + forget_leak
    key_gate = (1.0 - forget_floor) * jax.nn.sigmoid(-gate_logit)
    query_act = jax.nn.silu(proj_query.astype(jnp.float32))
    value_f = proj_input.astype(jnp.float32)
    nblk = count // BLOCK

    def to_blocks(arr):
        return arr.reshape(nblk, BLOCK, heads, GROUP_FEATURES).transpose(0, 2, 1, 3)
    start_state = jnp.zeros((heads, GROUP_FEATURES, GROUP_FEATURES), jnp.float32)
    _, outputs = lax.scan(state_block, start_state, (to_blocks(query_act), to_blocks(key_gate), to_blocks(value_f), to_blocks(log_forget)))
    state_read = outputs.transpose(0, 2, 1, 3).reshape(count, heads, GROUP_FEATURES)
    out_gate = jax.nn.silu(proj_outgate.astype(jnp.float32)).reshape(count, heads, GROUP_FEATURES)
    state_res = (rms_rows(state_read, state_gain) * out_gate).reshape(count, STATE_W).astype(jnp.bfloat16)
    conv_in = (proj_c.astype(jnp.float32) * proj_h.astype(jnp.float32)).astype(jnp.bfloat16)
    padded = jnp.concatenate([jnp.zeros((TAPS - 1, CONV_CH), jnp.bfloat16), conv_in], axis=0).astype(jnp.float32)
    taps_f = conv_taps.astype(jnp.float32)
    conv_sum = jnp.zeros((count, CONV_CH), jnp.float32)
    for offset in range(TAPS):
        conv_sum = conv_sum + taps_f[offset][None, :] * padded[offset:offset + count]
    gated = (proj_b.astype(jnp.float32) * conv_sum).reshape(count, CONV_CH // GROUP_FEATURES, GROUP_FEATURES)
    conv_res = rms_rows(gated, group_gain).reshape(count, CONV_CH).astype(jnp.bfloat16)
    total = jnp.dot(state_res, out_state, preferred_element_type=jnp.float32)
    total = total + jnp.dot(conv_res, out_conv, preferred_element_type=jnp.float32)
    return total.astype(jnp.bfloat16)
```

```python
import functools

import jax
import jax.numpy as jnp
from jax import lax
from jax.experimental import pallas as pl
from jax.experimental.pallas import tpu as pltpu
from jax.sharding import Mesh
from jax.sharding import PartitionSpec as P

F = 128
CH = 128
RB = 256
EPS = 1e-6
MESH = pl.DeviceIdType.MESH
F32, BF16 = jnp.float32, jnp.bfloat16
NT = (((1,), (1,)), ((), ()))
TN = (((0,), (0,)), ((), ()))


def mm(a, b):
    return jnp.dot(a, b, preferred_element_type=F32)


def mmg(a, b, dims):
    return lax.dot_general(a, b, dims, preferred_element_type=F32)


def silu(v):
    return v * jax.nn.sigmoid(v)


def kernel(
    NZ, NY, NX, T, D,
    tok_h, gain_h, wq_h, wf_h, wi_h, wo_h, wh_h, wb_h, wc_h, floor_h, leak_h, sgain_h, taps_h, ggain_h, ost_h, ocv_h,
    out,
    tok, xg, wfv, whc, wqo, wb, gain, floor, sgain, ggain, taps, leak, ost, ocv,
    rs, fbuf, km, vb, lbuf, sst, lst, qg, ol, gate, cpad, bproj,
    my, ry, mz, rz, mb, sin, rim, act, g, w, acc, osw,
    ld, ys, yr, zs, zr, bs, br, rms, rmr, as_, ar, rls, rlr, sbs, sbr, wss, wsr, wfs, wfr, oss, osr,
):
    z, y, x, c = (lax.axis_index(a) for a in ("z", "y", "x", "c"))
    H = T // 2
    nb, nc = T // RB, T // CH
    N = D // NX
    KC = 2 * F

    def rcopy(src, dst, ss, rsem, dev):
        return pltpu.make_async_remote_copy(
            src_ref=src, dst_ref=dst, send_sem=ss, recv_sem=rsem, device_id=dev, device_id_type=MESH
        )

    def arrived(dst, sem):
        rcopy(dst, dst, sem, sem, {"c": 1 - c}).wait_recv()

    def left(src, sem):
        rcopy(src, src, sem, sem, {"c": 1 - c}).wait_send()

    nxt_y = lax.rem(y + 1, NY)
    nxt_z = lax.rem(z + (y + 1) // NY, NZ)
    prv_y = lax.rem(y + NY - 1, NY)
    prv_z = lax.rem(z + NZ - (NY - y) // NY, NZ)
    nxt = {"z": nxt_z, "y": nxt_y}
    prv = {"z": prv_z, "y": prv_y}
    other = 1 - c

    bar = pltpu.get_barrier_semaphore()
    count = 0
    for d in range(1, NX):
        for e in range(2):
            pl.semaphore_signal(bar, inc=1, device_id={"x": lax.rem(x + d, NX), "c": e}, device_id_type=MESH)
            count += 1
    pl.semaphore_signal(bar, inc=1, device_id={"c": other}, device_id_type=MESH)
    for d in range(1, NY):
        pl.semaphore_signal(bar, inc=1, device_id={"y": lax.rem(y + d, NY)}, device_id_type=MESH)
    for d in range(1, NZ):
        pl.semaphore_signal(bar, inc=1, device_id={"z": lax.rem(z + d, NZ)}, device_id_type=MESH)
    pl.semaphore_signal(bar, inc=1, device_id=nxt, device_id_type=MESH)
    pl.semaphore_signal(bar, inc=1, device_id=prv, device_id_type=MESH)
    count += 1 + (NY - 1) + (NZ - 1) + 2

    lds = {}

    def load(name, src, dst):
        cp = pltpu.make_async_copy(src, dst, ld.at[len(lds)])
        lds[name] = cp
        cp.start()

    def need(*names):
        for name in names:
            lds[name].wait()

    def rows(i, n):
        return pl.ds(i * n, n)

    load("gain", gain_h, gain)
    load("t0", tok_h.at[rows(0, RB)], tok.at[rows(0, RB)])
    load("wf", wf_h, wfv.at[:, 0:F])
    load("wi", wi_h, wfv.at[:, F : 2 * F])
    for i in range(1, nb):
        load(f"t{i}", tok_h.at[rows(i, RB)], tok.at[rows(i, RB)])
    load("floor", floor_h, floor)
    load("leak", leak_h, leak)
    load("ocv", ocv_h, ocv)
    load("ost", ost_h, ost)

    def prep(i):
        r = rows(i, RB)
        for k in range(RB // 64):
            q = pl.ds(i * RB + k * 64, 64)
            t = tok[q, :].astype(F32)
            xg[q, :] = (t * gain[...]).astype(BF16)
            ms = jnp.sum(t * t, axis=-1, keepdims=True) * (1.0 / D)
            rs[q, :] = jnp.broadcast_to(lax.rsqrt(ms + EPS), (64, F))

    def fv(i):
        r = rows(i, RB)
        p = mm(xg[r, :], wfv[...])
        s = rs[r, :]
        fbuf[r, :] = p[:, 0:F] * s
        vb[r, :] = (p[:, F : 2 * F] * s).astype(BF16)

    ri = lax.broadcasted_iota(jnp.int32, (CH, CH), 0)
    ci = lax.broadcasted_iota(jnp.int32, (CH, CH), 1)
    causal = ri >= ci
    tri = jnp.where(causal, 1.0, 0.0).astype(BF16)

    def block(i, state, start):
        r = rows(i, CH)
        k = (1.0 - floor[...]) * jax.nn.sigmoid(-fbuf[r, :])
        lf = jnp.log1p(-k) + leak[r, :]
        hi = lf.astype(BF16)
        lo = (lf - hi.astype(F32)).astype(BF16)
        two = mm(tri, jnp.concatenate([hi, lo], axis=1))
        cum = two[:, 0:F] + two[:, F : 2 * F]
        total = cum[CH - 1 : CH, :]
        mid = cum[CH // 2 - 1 : CH // 2, :]
        lbuf[r, :] = cum
        lst[i] = jnp.broadcast_to(start, (8, F))
        km[r, :] = (k * jnp.exp(mid - cum)).astype(BF16)
        kd = (k * jnp.exp(total - cum)).astype(BF16)
        sst[i] = state.astype(BF16)
        state = state * jnp.exp(total) + mmg(vb[r, :], kd, TN)
        return state, start + total

    state, start = jnp.zeros((F, F), F32), jnp.zeros((1, F), F32)
    need("gain", "t0")
    prep(0)
    need("wf", "wi")
    per = RB // CH
    for i in range(nb):
        if i + 1 < nb:
            need(f"t{i + 1}")
        if i == 0:
            load("wh", wh_h, whc.at[:, 0:F])
            load("wc", wc_h, whc.at[:, F : 2 * F])
            load("wb", wb_h, wb)
            load("taps", taps_h, taps)
            load("ggain", ggain_h, ggain)
            load("wq", wq_h, wqo.at[:, 0:F])
            load("wo", wo_h, wqo.at[:, F : 2 * F])
            load("sgain", sgain_h, sgain)
        if i == 1:
            need("floor", "leak")
        fv(i)
        if i + 1 < nb:
            prep(i + 1)
        if i >= 1:
            for j in range((i - 1) * per, i * per):
                state, start = block(j, state, start)
        if i == 1:
            need("ocv", "ost")
            pl.semaphore_wait(bar, count)
            for kind, src in ((0, ocv), (1, ost)):
                place = lambda slot: w.at[pl.ds(kind * NX * KC + slot * KC + c * F, F), :]
                for d, slot in ((1, 1), (NX - 1, 2), (2, 3)):
                    to = lax.rem(x + d, NX)
                    rcopy(
                        src.at[:, pl.ds(pl.multiple_of(to * N, N), N)], place(slot),
                        wss.at[kind, slot], wsr.at[kind, slot], {"x": to},
                    ).start()
                mine = src.at[:, pl.ds(pl.multiple_of(x * N, N), N)]
                rcopy(mine, place(0), wfs.at[kind, 0], wfr.at[kind, 0], {"c": other}).start()
                w[pl.ds(pl.multiple_of(kind * NX * KC + c * F, F), F), :] = src[:, pl.ds(pl.multiple_of(x * N, N), N)]
    for j in range((nb - 1) * per, nc):
        state, start = block(j, state, start)

    Q = F // NY
    r16 = lax.broadcasted_iota(jnp.int32, (16, F), 0)

    def decay_rows(dec):
        top = dec.astype(BF16)
        low = (dec - top.astype(F32)).astype(BF16)
        return jnp.where(r16 == 0, top.astype(F32), low.astype(F32)).astype(BF16)

    drow = decay_rows(jnp.exp(start))
    for q in range(NY):
        my[q, 0:Q, :] = state[q * Q : (q + 1) * Q, :].astype(BF16)
        my[q, Q : Q + 16, :] = drow
    ry[y] = my[y]
    for d in range(1, NY):
        to = lax.rem(y + d, NY)
        rcopy(my.at[to], ry.at[y], ys.at[d], yr.at[d], {"y": to}).start()

    need("wh", "wc", "wb", "taps", "ggain")

    def hcb(i):
        r = rows(i, RB)
        s = rs[r, :]
        p = mm(xg[r, :], whc[...])
        cpad[pl.ds(8 + i * RB, RB), :] = ((p[:, 0:F] * s) * (p[:, F : 2 * F] * s)).astype(BF16).astype(F32)
        bproj[r, :] = mm(xg[r, :], wb[...]) * s

    hcb(nb - 1)
    rcopy(cpad.at[pl.ds(T, 8), :], rim, rms.at[0], rmr.at[0], nxt).start()
    for i in range(nb - 2, -1, -1):
        hcb(i)

    tf = taps[...].astype(F32)

    def conv(i):
        r = rows(i, RB)
        total = tf[0:1, :] * cpad[pl.ds(6 + i * RB, RB), :]
        total = total + tf[1:2, :] * cpad[pl.ds(7 + i * RB, RB), :]
        total = total + tf[2:3, :] * cpad[pl.ds(8 + i * RB, RB), :]
        v = bproj[r, :] * total
        ms = jnp.mean(v * v, axis=-1, keepdims=True)
        act[0, r, :] = (v * lax.rsqrt(ms + EPS) * ggain[...]).astype(BF16)

    for i in range(nb - 1, 0, -1):
        conv(i)

    def part(ref, k):
        dec = ref[k, Q : Q + 16, :].astype(F32)
        return ref[k, 0:Q, :].astype(F32), dec[0:1, :] + dec[1:2, :]

    for d in range(1, NY):
        arrived(ry.at[0], yr.at[d])
    ps, pd = [jnp.zeros((Q, F), F32)], [jnp.ones((1, F), F32)]
    for k in range(NY):
        s, dec = part(ry, k)
        ps.append(ps[k] * dec + s)
        pd.append(pd[k] * dec)
    mz[0:Q, :] = ps[NY].astype(BF16)
    mz[Q : Q + 16, :] = decay_rows(pd[NY])
    rz[z] = mz[...]
    for d in range(1, NZ):
        to = lax.rem(z + d, NZ)
        rcopy(mz, rz.at[z], zs.at[d], zr.at[d], {"z": to}).start()

    arrived(rim, rmr.at[0])
    cpad[0:8, :] = jnp.where(z + y == 0, 0.0, rim[...])
    conv(0)

    def gcol(kind, slot):
        return kind * NX * KC + slot * KC

    def spread(kind):
        for k in range(2):
            for way in range(2):
                part_k = k if way == 0 else 1 - k
                to = lax.rem(x + (1 if way == 0 else NX - 1), NX)
                for e in range(2):
                    rcopy(
                        act.at[kind, pl.ds(e * H + part_k * RB, RB), :],
                        g.at[pl.ds(part_k * RB, RB), pl.ds(pl.multiple_of(gcol(kind, 1 + way) + c * F, F), F)],
                        as_.at[kind, way, part_k, e], ar.at[kind, way, part_k, c], {"x": to, "c": e},
                    ).start()
            if k == 0:
                rcopy(
                    act.at[kind, pl.ds(pl.multiple_of(other * H, H), H), :],
                    g.at[:, pl.ds(pl.multiple_of(gcol(kind, 0) + c * F, F), F)],
                    sbs.at[kind], sbr.at[kind], {"c": other},
                ).start()
        g[:, pl.ds(pl.multiple_of(gcol(kind, 0) + c * F, F), F)] = act[kind, pl.ds(pl.multiple_of(c * H, H), H), :]

    def gblock(kind, slot, part_k, e):
        return g.at[pl.ds(part_k * RB, RB), pl.ds(gcol(kind, slot) + e * F, F)]

    def relayed(kind, way):
        part_k = way
        to = lax.rem(x + (1 if way == 0 else NX - 1), NX)
        for e in range(2):
            arrived(gblock(kind, 1 + way, part_k, e), ar.at[kind, way, part_k, e])
        rcopy(
            g.at[pl.ds(part_k * RB, RB), pl.ds(gcol(kind, 1 + way), KC)],
            g.at[pl.ds(part_k * RB, RB), pl.ds(gcol(kind, 3), KC)],
            rls.at[kind, way], rlr.at[kind, way], {"x": to},
        ).start()

    def gathered_near(kind):
        for way in range(2):
            part_k = 1 - way
            for e in range(2):
                arrived(gblock(kind, 1 + way, part_k, e), ar.at[kind, way, part_k, e])
        arrived(g.at[:, pl.ds(0, F)], sbr.at[kind])

    def gathered_far(kind, way):
        arrived(g.at[pl.ds(way * RB, RB), pl.ds(gcol(kind, 3), KC)], rlr.at[kind, way])

    spread(0)

    need("wq", "wo", "sgain")

    def qo(i):
        r = rows(i, RB)
        s = rs[r, :]
        p = mm(xg[r, :], wqo[...])
        fbuf[r, :] = silu(p[:, 0:F] * s)
        gate[r, :] = silu(p[:, F : 2 * F] * s) * sgain[...]

    def reads(i):
        r = rows(i, CH)
        cum = lbuf[r, :]
        q = fbuf[r, :]
        mid = cum[CH // 2 - 1 : CH // 2, :]
        qm = (q * jnp.exp(cum - mid)).astype(BF16)
        ql = (q * jnp.exp(cum)).astype(BF16)
        qg[r, :] = (q * jnp.exp(cum + lst[i][0:1, :])).astype(BF16)
        scores = jnp.where(causal, mmg(qm, km[r, :], NT), 0.0).astype(BF16)
        ol[r, :] = mm(scores, vb[r, :]) + mmg(ql, sst[i], NT)

    for i in range(nb):
        qo(i)
        if i >= 1:
            for j in range((i - 1) * per, i * per):
                reads(j)
    for j in range((nb - 1) * per, nc):
        reads(j)

    for kind in range(2):
        for slot in range(1, 4):
            place = w.at[pl.ds(kind * NX * KC + slot * KC + c * F, F), :]
            arrived(place, wsr.at[kind, slot])
            rcopy(place, place, wfs.at[kind, slot], wfr.at[kind, slot], {"c": other}).start()

    for d in range(1, NZ):
        arrived(rz.at[0], zr.at[d])
    before = jnp.zeros((Q, F), F32)
    for k in range(NZ - 1):
        s, dec = part(rz, k)
        before = jnp.where(k < z, before * dec + s, before)
    for k in range(NY):
        mb[k] = (before * pd[k] + ps[k]).astype(BF16)
    mine = pl.ds(pl.multiple_of(y * Q, Q), Q)
    sin[mine, :] = mb[y]
    for d in range(1, NY):
        to = lax.rem(y + d, NY)
        rcopy(mb.at[to], sin.at[mine, :], bs.at[d], br.at[d], {"y": to}).start()

    relayed(0, 0)
    relayed(0, 1)

    for d in range(1, NY):
        arrived(sin.at[0:Q, :], br.at[d])

    def finish(i):
        r = rows(i, RB)
        v = ol[r, :] + mmg(qg[r, :], sin[...], NT)
        ms = jnp.mean(v * v, axis=-1, keepdims=True)
        act[1, r, :] = (v * lax.rsqrt(ms + EPS) * gate[r, :]).astype(BF16)

    for i in range(nb):
        finish(i)
    spread(1)

    for kind in range(2):
        for slot in range(4):
            arrived(w.at[pl.ds(0, F), :], wfr.at[kind, slot])
    gathered_near(0)
    for way in range(2):
        gathered_far(0, way)
        r = rows(way, RB)
        acc[r, :] = mm(g[r, 0 : NX * KC], w[0 : NX * KC, :])
    relayed(1, 0)
    relayed(1, 1)
    gathered_near(1)
    for way in range(2):
        r = rows(way, RB)
        acc[r, :] = acc[r, :] + mm(g[r, gcol(1, 0) : gcol(1, 3)], w[gcol(1, 0) : gcol(1, 3), :])
    for way in range(2):
        gathered_far(1, way)
        r = rows(way, RB)
        res = (acc[r, :] + mm(g[r, gcol(1, 3) : gcol(1, 4)], w[gcol(1, 3) : gcol(1, 4), :])).astype(BF16)
        first = res[:, 0 : N // 2]
        second = res[:, N // 2 : N]
        osw[r, :] = jnp.where(c == 0, second.astype(F32), first.astype(F32)).astype(BF16)
        o = pl.ds(pl.multiple_of(c * H + way * RB, RB), RB)
        rcopy(osw.at[r, :], out.at[o, :], oss.at[way], osr.at[way], {"c": other}).start()
        out[o, :] = jnp.where(c == 0, first.astype(F32), second.astype(F32)).astype(BF16)

    for d in range(1, NY):
        left(my.at[0], ys.at[d])
        left(mb.at[0], bs.at[d])
    for d in range(1, NZ):
        left(mz, zs.at[d])
    left(rim, rms.at[0])
    for kind in range(2):
        for way in range(2):
            for k in range(2):
                for e in range(2):
                    left(act.at[kind, 0:RB, :], as_.at[kind, way, k, e])
            left(g.at[0:RB, 0:KC], rls.at[kind, way])
        left(act.at[kind, 0:H, :], sbs.at[kind])
        for slot in range(4):
            if slot:
                left(w.at[0:F, :], wss.at[kind, slot])
            left(w.at[0:F, :], wfs.at[kind, slot])
    for way in range(2):
        left(osw.at[0:RB, :], oss.at[way])
        arrived(out.at[0:RB, :], osr.at[way])


def body(NZ, NY, NX, *args):
    (tokens, in_gain, wq, wf, wi, wo, wh, wb, wc, floor, leak, sgain, taps, ggain, ost, ocv) = args
    T, D = tokens.shape
    N = D // NX
    row = lambda a: a.reshape(1, -1)
    V, S = pltpu.VMEM, pltpu.SemaphoreType.DMA
    nc = T // CH
    Q = F // NY
    scratch = [
        V((T, D), BF16), V((T, D), BF16),
        V((D, 2 * F), BF16), V((D, 2 * F), BF16), V((D, 2 * F), BF16), V((D, F), BF16),
        V((1, D), F32), V((1, F), F32), V((1, F), F32), V((1, F), F32), V((3, F), BF16),
        V((T, F), F32), V((F, D), BF16), V((F, D), BF16),
        V((T, F), F32), V((T, F), F32), V((T, F), BF16), V((T, F), BF16), V((T, F), F32),
        V((nc, F, F), BF16), V((nc, 8, F), F32), V((T, F), BF16), V((T, F), F32), V((T, F), F32),
        V((T + 8, F), F32), V((T, F), F32),
        V((NY, Q + 16, F), BF16), V((NY, Q + 16, F), BF16), V((Q + 16, F), BF16), V((NZ, Q + 16, F), BF16),
        V((NY, Q, F), BF16), V((F, F), BF16), V((8, F), F32), V((2, T, F), BF16),
        V((T // 2, 4 * F * NX), BF16), V((4 * F * NX, N), BF16), V((T // 2, N), F32), V((T // 2, N // 2), BF16),
        S((24,)), S((NY,)), S((NY,)), S((NZ,)), S((NZ,)), S((NY,)), S((NY,)), S((1,)), S((1,)),
        S((2, 2, 2, 2)), S((2, 2, 2, 2)), S((2, 2)), S((2, 2)), S((2,)), S((2,)),
        S((2, 4)), S((2, 4)), S((2, 4)), S((2, 4)), S((2,)), S((2,)),
    ]
    return pl.pallas_call(
        functools.partial(kernel, NZ, NY, NX, T, D),
        name="mixer",
        out_shape=jax.ShapeDtypeStruct((T, N // 2), BF16),
        in_specs=[pl.BlockSpec(memory_space=pl.ANY)] * 16,
        out_specs=pl.BlockSpec(memory_space=pltpu.VMEM),
        scratch_shapes=scratch,
        compiler_params=pltpu.CompilerParams(
            collective_id=0, has_side_effects=True, vmem_limit_bytes=58 * 1024 * 1024
        ),
    )(
        tokens, row(in_gain), wq, wf, wi, wo, wh, wb, wc, row(floor), leak, row(sgain), taps, row(ggain), ost, ocv
    )


def solution(mesh):
    NZ, NY, NX = 8, 4, 4
    split = Mesh(mesh.devices.reshape(NZ, NY, NX, 2), ("z", "y", "x", "c"))
    sp, tp = ("z", "y"), ("x", "c")
    wide = P(None, tp)
    placed = (
        P(sp, None), P(), wide, wide, wide, wide, wide, wide, wide, P(tp), P(sp, tp), P(), wide, P(), P(tp, None), P(tp, None),
    )
    return jax.shard_map(
        functools.partial(body, NZ, NY, NX), mesh=split, in_specs=placed, out_specs=P(sp, tp), check_vma=False
    )
```

```python
import functools

import jax
import jax.numpy as jnp
from jax import lax
from jax.experimental import pallas as pl
from jax.experimental.pallas import tpu as pltpu
from jax.sharding import Mesh
from jax.sharding import PartitionSpec as P

F = 128
CH = 128
RB = 256
EPS = 1e-6
MESH = pl.DeviceIdType.MESH
F32, BF16 = jnp.float32, jnp.bfloat16
NT = (((1,), (1,)), ((), ()))
TN = (((0,), (0,)), ((), ()))


def mm(a, b):
    return jnp.dot(a, b, preferred_element_type=F32)


def mmg(a, b, dims):
    return lax.dot_general(a, b, dims, preferred_element_type=F32)


LOG_TERMS = (1.000000000114827, 0.49999993460512276, 0.33333939010389413, 0.24979093708816186, 0.20339952431978914, 0.13889282460472627, 0.24939632181800545)


def log_part(k):
    p = jnp.full_like(k, LOG_TERMS[-1])
    for term in LOG_TERMS[-2::-1]:
        p = p * k + term
    return p * k


def far_first(n):
    return sorted(range(1, n), key=lambda d: (-min(d, n - d), d))


def silu(v):
    return v * jax.nn.sigmoid(v)


def kernel(
    NZ, NY, NX, T, D,
    tok_h, gain_h, wq_h, wf_h, wi_h, wo_h, wh_h, wb_h, wc_h, floor_h, leak_h, sgain_h, taps_h, ggain_h, ost_h, ocv_h,
    out,
    tok, wfv, wrest, gain, gcol, small, taps, leak, wout,
    rs, fbuf, km, vb, lbuf, sst, lst, qg, ol, gate, cpad, bproj,
    my, ry, mz, rz, mb, sin, rim, act, g, w, acc, osw,
    ld, xr, ar, rlr, sbr, w1r, w2r, w3r, wfr, osr, sends,
):
    z, y, x, c = (lax.axis_index(a) for a in ("z", "y", "x", "c"))
    H = T // 2
    nb, nc = T // RB, T // CH
    N = D // NX
    KC = 2 * F

    def rcopy(src, dst, ss, rsem, dev):
        return pltpu.make_async_remote_copy(
            src_ref=src, dst_ref=dst, send_sem=ss, recv_sem=rsem, device_id=dev, device_id_type=MESH
        )

    def arrived(dst, sem):
        rcopy(dst, dst, sem, sem, {"c": 1 - c}).wait_recv()

    def left(src, sem):
        rcopy(src, src, sem, sem, {"c": 1 - c}).wait_send()

    nxt_y = lax.rem(y + 1, NY)
    nxt_z = lax.rem(z + (y + 1) // NY, NZ)
    prv_y = lax.rem(y + NY - 1, NY)
    prv_z = lax.rem(z + NZ - (NY - y) // NY, NZ)
    nxt = {"z": nxt_z, "y": nxt_y}
    prv = {"z": prv_z, "y": prv_y}
    other = 1 - c
    sent, sent_s, sent_z = sends.at[0], sends.at[1], sends.at[2]

    lds = {}

    def load(name, whole, *pairs):
        sem = ld.at[len(lds)]
        lds[name] = whole, sem
        for src, dst in pairs:
            pltpu.make_async_copy(src, dst, sem).start()

    def need(*names):
        for name in names:
            whole, sem = lds[name]
            pltpu.make_async_copy(whole, whole, sem).wait()

    def rows(i, n):
        return pl.ds(i * n, n)

    def load_rows(i):
        r = rows(i, RB)
        load(f"t{i}", tok.at[r], (tok_h.at[r], tok.at[r]))

    def load_pair(name, ref, left_h, right_h):
        load(name, ref, (left_h, ref.at[:, 0:F]), (right_h, ref.at[:, F : 2 * F]))

    def load_pair(ref, at, left_h, right_h):
        return (left_h, ref.at[:, at : at + F]), (right_h, ref.at[:, at + F : at + 2 * F])

    HALF = pl.ds(T // 2, T // 2)
    load("gain", gain, (gain_h, gain))
    load("t0", tok.at[0:RB], (tok_h.at[0:RB], tok.at[0:RB]))
    load("wfv", wfv, *load_pair(wfv, 0, wf_h, wi_h))
    load("t1", tok.at[RB : 2 * RB], (tok_h.at[RB : 2 * RB], tok.at[RB : 2 * RB]))
    load("small", small, (floor_h, small.at[0]), (sgain_h, small.at[1]), (ggain_h, small.at[2]))
    load("t2", tok.at[HALF], (tok_h.at[HALF], tok.at[HALF]))
    load("leak", leak, (leak_h, leak))
    load("wout", wout, (ocv_h, wout.at[0]), (ost_h, wout.at[1]))

    bar = pltpu.get_barrier_semaphore()
    count = 0
    for d in range(1, NX):
        for e in range(2):
            pl.semaphore_signal(bar, inc=1, device_id={"x": lax.rem(x + d, NX), "c": e}, device_id_type=MESH)
            count += 1
    pl.semaphore_signal(bar, inc=1, device_id={"c": other}, device_id_type=MESH)
    for d in range(1, NY):
        pl.semaphore_signal(bar, inc=1, device_id={"y": lax.rem(y + d, NY)}, device_id_type=MESH)
    for d in range(1, NZ):
        pl.semaphore_signal(bar, inc=1, device_id={"z": lax.rem(z + d, NZ)}, device_id_type=MESH)
    pl.semaphore_signal(bar, inc=1, device_id=nxt, device_id_type=MESH)
    pl.semaphore_signal(bar, inc=1, device_id=prv, device_id_type=MESH)
    count += 1 + (NY - 1) + (NZ - 1) + 2

    def turn_gain():
        for k in range(D // F):
            r = rows(k, F)
            gcol[r, :] = jnp.transpose(jnp.broadcast_to(gain[:, k * F : (k + 1) * F], (F, F)))

    def scale(ref):
        for k in range(D // F):
            r = rows(k, F)
            for n in range(ref.shape[1] // F):
                v = ref[r, n * F : (n + 1) * F].astype(F32) * gcol[r, :]
                ref[r, n * F : (n + 1) * F] = v.astype(BF16)

    def norms(i):
        for k in range(RB // 64):
            q = pl.ds(i * RB + k * 64, 64)
            t = tok[q, :].astype(F32)
            ms = jnp.sum(t * t, axis=-1, keepdims=True) * (1.0 / D)
            rs[q, :] = jnp.broadcast_to(lax.rsqrt(ms + EPS), (64, F))

    def fv(i):
        r = rows(i, T // 2)
        p = mm(tok[r, :], wfv[...])
        s = rs[r, :]
        fbuf[r, :] = p[:, 0:F] * s
        vb[r, :] = (p[:, F : 2 * F] * s).astype(BF16)

    ri = lax.broadcasted_iota(jnp.int32, (CH, CH), 0)
    ci = lax.broadcasted_iota(jnp.int32, (CH, CH), 1)
    causal = ri >= ci
    tri = jnp.where(causal, 1.0, 0.0).astype(BF16)

    def block(i, state, start):
        r = rows(i, CH)
        k = (1.0 - small[0]) * jax.nn.sigmoid(-fbuf[r, :])
        lf = leak[r, :] - log_part(k)
        hi = lf.astype(BF16)
        lo = (lf - hi.astype(F32)).astype(BF16)
        two = mm(tri, jnp.concatenate([hi, lo], axis=1))
        cum = two[:, 0:F] + two[:, F : 2 * F]
        total = cum[CH - 1 : CH, :]
        mid = cum[CH // 2 - 1 : CH // 2, :]
        lbuf[r, :] = cum
        lst[i] = jnp.broadcast_to(start, (8, F))
        kmid = k * jnp.exp(mid - cum)
        km[r, :] = kmid.astype(BF16)
        kd = (kmid * jnp.exp(total - mid)).astype(BF16)
        sst[i] = state.astype(BF16)
        state = state * jnp.exp(total) + mmg(vb[r, :], kd, TN)
        return state, start + total

    state, start = jnp.zeros((F, F), F32), jnp.zeros((1, F), F32)
    Q = F // NY
    wpart = pl.ds(pl.multiple_of(y * Q, Q), Q)
    wmine = pl.ds(pl.multiple_of(c * F + y * Q, Q), Q)
    wcore = pl.ds(pl.multiple_of(c * F, F), F)

    def wspread(kind):
        part_w = w.at[kind, 1:NX, wmine, :]
        for d in (1, NY - 1):
            rcopy(part_w, part_w, sent, w2r.at[kind], {"y": lax.rem(y + d, NY)}).start()

    def wrelay(kind):
        arrived(w.at[kind, 1:NX, 0 : 2 * Q, :], w2r.at[kind])
        for d in (1, NY - 1):
            source = lax.rem(y + NY - d, NY)
            at = c * F + source * Q + (0 if d == 1 else Q // 2)
            part_w = w.at[kind, 1:NX, pl.ds(pl.multiple_of(at, Q // 2), Q // 2), :]
            rcopy(part_w, part_w, sent, w3r.at[kind], {"y": lax.rem(y + d, NY)}).start()

    def wforward(kind):
        arrived(w.at[kind, 1:NX, 0:Q, :], w3r.at[kind])
        part_w = w.at[kind, 1:NX, wcore, :]
        rcopy(part_w, part_w, sent, wfr.at[kind], {"c": other}).start()
    with jax.named_scope("head"):
        need("gain")
        turn_gain()
        need("t0")
        norms(0)
        need("wfv")
        scale(wfv)
        need("t1")
        norms(1)
    per = RB // CH
    with jax.named_scope("first"):
        fv(0)
    need("t2", "small", "leak")
    load("wrest", wrest, *load_pair(wrest, 0, wh_h, wc_h), (wb_h, wrest.at[:, 2 * F : 3 * F]), *load_pair(wrest, 3 * F, wq_h, wo_h))
    load("taps", taps, (taps_h, taps))
    with jax.named_scope("first"):
        norms(2)
        norms(3)
        fv(1)
        for j in range(nc // 2):
            state, start = block(j, state, start)
    with jax.named_scope("barrier_wait"):
        need("wout")
        pl.semaphore_wait(bar, count)
    for kind in range(2):
        for d, slot in ((2, 3), (1, 1), (NX - 1, 2)):
            to = lax.rem(x + d, NX)
            rcopy(
                wout.at[kind, wpart, pl.ds(pl.multiple_of(to * N, N), N)],
                w.at[kind, slot, wmine, :], sent, w1r.at[0], {"x": to},
            ).start()
        own = wout.at[kind, :, pl.ds(pl.multiple_of(x * N, N), N)]
        rcopy(own, w.at[kind, 0, wcore, :], sent, wfr.at[kind], {"c": other}).start()
    with jax.named_scope("last_blocks"):
        for j in range(nc // 2, nc):
            state, start = block(j, state, start)

    r16 = lax.broadcasted_iota(jnp.int32, (16, F), 0)

    def decay_rows(dec):
        top = dec.astype(BF16)
        low = (dec - top.astype(F32)).astype(BF16)
        return jnp.where(r16 == 0, top.astype(F32), low.astype(F32)).astype(BF16)

    drow = decay_rows(jnp.exp(start))
    for q in range(NY):
        my[q, 0:Q, :] = state[q * Q : (q + 1) * Q, :].astype(BF16)
        my[q, Q : Q + 16, :] = drow
    ry[y] = my[y]
    for d in far_first(NY):
        to = lax.rem(y + d, NY)
        rcopy(my.at[to], ry.at[y], sent_s, xr.at[0], {"y": to}).start()

    for kind in range(2):
        w[kind, 0, wcore, :] = wout[kind, :, pl.ds(pl.multiple_of(x * N, N), N)]

    with jax.named_scope("w_wait"):
        need("wrest", "taps")
    scale(wrest.at[:, 0 : 3 * F])

    def hcb(i):
        r = rows(i, RB)
        s = rs[r, :]
        p = mm(tok[r, :], wrest[:, 0 : 2 * F])
        cpad[pl.ds(8 + i * RB, RB), :] = ((p[:, 0:F] * s) * (p[:, F : 2 * F] * s)).astype(BF16).astype(F32)
        bproj[r, :] = mm(tok[r, :], wrest[:, 2 * F : 3 * F]) * s

    hcb(nb - 1)
    rcopy(cpad.at[pl.ds(T, 8), :], rim, sent_s, xr.at[3], nxt).start()
    with jax.named_scope("hcb"):
        for i in range(nb - 2, -1, -1):
            hcb(i)

    tf = taps[...].astype(F32)

    def conv(i):
        r = rows(i, RB)
        total = tf[0:1, :] * cpad[pl.ds(6 + i * RB, RB), :]
        total = total + tf[1:2, :] * cpad[pl.ds(7 + i * RB, RB), :]
        total = total + tf[2:3, :] * cpad[pl.ds(8 + i * RB, RB), :]
        v = bproj[r, :] * total
        ms = jnp.mean(v * v, axis=-1, keepdims=True)
        act[0, r, :] = (v * lax.rsqrt(ms + EPS) * small[2]).astype(BF16)

    with jax.named_scope("conv"):
        for i in range(nb - 1, 0, -1):
            conv(i)

    scale(wrest.at[:, 3 * F : 5 * F])

    def qo(i):
        r = rows(i, RB)
        s = rs[r, :]
        p = mm(tok[r, :], wrest[:, 3 * F : 5 * F])
        fbuf[r, :] = silu(p[:, 0:F] * s)
        gate[r, :] = silu(p[:, F : 2 * F] * s) * small[1]

    def reads(i):
        r = rows(i, CH)
        cum = lbuf[r, :]
        q = fbuf[r, :]
        mid = cum[CH // 2 - 1 : CH // 2, :]
        qmid = q * jnp.exp(cum - mid)
        qm = qmid.astype(BF16)
        ql = (qmid * jnp.exp(mid)).astype(BF16)
        qg[r, :] = (qmid * jnp.exp(mid + lst[i][0:1, :])).astype(BF16)
        scores = jnp.where(causal, mmg(qm, km[r, :], NT), 0.0).astype(BF16)
        ol[r, :] = mm(scores, vb[r, :]) + mmg(ql, sst[i], NT)

    with jax.named_scope("qo"):
        qo(0)
        qo(1)
        for j in range(per):
            reads(j)

    def part(ref, k):
        dec = ref[k, Q : Q + 16, :].astype(F32)
        return ref[k, 0:Q, :].astype(F32), dec[0:1, :] + dec[1:2, :]

    with jax.named_scope("s1_wait"):
        arrived(ry.at[0 : NY - 1], xr.at[0])
    ps, pd = [jnp.zeros((Q, F), F32)], [jnp.ones((1, F), F32)]
    for k in range(NY):
        s, dec = part(ry, k)
        ps.append(ps[k] * dec + s)
        pd.append(pd[k] * dec)
    mz[0:Q, :] = ps[NY].astype(BF16)
    mz[Q : Q + 16, :] = decay_rows(pd[NY])
    for d in far_first(NZ):
        @pl.when(z + d < NZ)
        def _():
            rcopy(mz, rz.at[z], sent_z, xr.at[1], {"z": lax.rem(z + d, NZ)}).start()

    with jax.named_scope("qo"):
        for i in range(2, nb):
            qo(i)
            for j in range((i - 1) * per, i * per):
                reads(j)
        for j in range((nb - 1) * per, nc):
            reads(j)

    with jax.named_scope("wspread"):
        arrived(w.at[0:2, 1:NX, 0:Q, :], w1r.at[0])
        wspread(0)
        wspread(1)

    with jax.named_scope("rim_wait"):
        arrived(rim, xr.at[3])
    cpad[0:8, :] = jnp.where(z + y == 0, 0.0, rim[...])
    conv(0)

    def gat(kind, slot):
        return kind * NX * KC + slot * KC

    def send(kind, way, part_k):
        to = lax.rem(x + (1 if way == 0 else NX - 1), NX)
        for e in range(2):
            rcopy(
                act.at[kind, pl.ds(e * H + part_k * RB, RB), :],
                g.at[pl.ds(part_k * RB, RB), pl.ds(pl.multiple_of(gat(kind, 1 + way) + c * F, F), F)],
                sent, ar.at[kind, way, part_k], {"x": to, "c": e},
            ).start()

    def keep(kind):
        place = g.at[:, pl.ds(pl.multiple_of(gat(kind, 0) + c * F, F), F)]
        rcopy(
            act.at[kind, pl.ds(pl.multiple_of(other * H, H), H), :], place, sent, sbr.at[kind], {"c": other}
        ).start()
        place[...] = act[kind, pl.ds(pl.multiple_of(c * H, H), H), :]

    def gblock(kind, slot, part_k):
        return g.at[pl.ds(part_k * RB, RB), pl.ds(gat(kind, slot), KC)]

    def relayed(kind, way):
        part_k = way
        to = lax.rem(x + (1 if way == 0 else NX - 1), NX)
        arrived(gblock(kind, 1 + way, part_k), ar.at[kind, way, part_k])
        rcopy(
            g.at[pl.ds(part_k * RB, RB), pl.ds(gat(kind, 1 + way), KC)],
            g.at[pl.ds(part_k * RB, RB), pl.ds(gat(kind, 3), KC)],
            sent, rlr.at[kind, way], {"x": to},
        ).start()

    def gathered_near(kind):
        for way in range(2):
            part_k = 1 - way
            arrived(gblock(kind, 1 + way, part_k), ar.at[kind, way, part_k])
        arrived(g.at[:, pl.ds(0, F)], sbr.at[kind])

    def gathered_far(kind, way):
        arrived(g.at[pl.ds(way * RB, RB), pl.ds(gat(kind, 3), KC)], rlr.at[kind, way])

    with jax.named_scope("spread0"):
        send(0, 0, 0)
        send(0, 1, 1)
        send(0, 0, 1)
        send(0, 1, 0)
        keep(0)

    with jax.named_scope("s2_wait"):
        for n in range(1, NZ):
            @pl.when(z == n)
            def _():
                arrived(rz.at[0:n], xr.at[1])
    before = jnp.zeros((Q, F), F32)
    for k in range(NZ - 1):
        s, dec = part(rz, k)
        before = jnp.where(k < z, before * dec + s, before)
    for k in range(NY):
        mb[k] = (before * pd[k] + ps[k]).astype(BF16)
    mine = pl.ds(pl.multiple_of(y * Q, Q), Q)
    sin[mine, :] = mb[y]
    for d in far_first(NY):
        to = lax.rem(y + d, NY)
        rcopy(mb.at[to], sin.at[mine, :], sent_s, xr.at[2], {"y": to}).start()

    with jax.named_scope("wrelay0"):
        wrelay(0)
    with jax.named_scope("relay0"):
        relayed(0, 0)
        relayed(0, 1)

    with jax.named_scope("s3_wait"):
        arrived(sin.at[0 : F - Q, :], xr.at[2])

    def finish(i):
        r = rows(i, RB)
        v = ol[r, :] + mmg(qg[r, :], sin[...], NT)
        ms = jnp.mean(v * v, axis=-1, keepdims=True)
        act[1, r, :] = (v * lax.rsqrt(ms + EPS) * gate[r, :]).astype(BF16)

    with jax.named_scope("finish"):
        finish(0)
        finish(2)
        send(1, 0, 0)
        finish(1)
        finish(3)
        send(1, 1, 1)
        send(1, 0, 1)
        send(1, 1, 0)
        keep(1)

    with jax.named_scope("wfr_near0"):
        wforward(0)
        wrelay(1)
        gathered_near(0)
        arrived(w.at[0, :, 0:F, :], wfr.at[0])
    for way in range(2):
        with jax.named_scope("far0"):
            gathered_far(0, way)
        r = rows(way, RB)
        acc[r, :] = mm(g[r, 0 : NX * KC], w[0].reshape(NX * KC, N))
    with jax.named_scope("relay1"):
        relayed(1, 0)
        relayed(1, 1)
    with jax.named_scope("wforward1"):
        wforward(1)
    with jax.named_scope("near1"):
        gathered_near(1)
        arrived(w.at[1, :, 0:F, :], wfr.at[1])
    for way in range(2):
        r = rows(way, RB)
        acc[r, :] = acc[r, :] + mm(g[r, gat(1, 0) : gat(1, 3)], w[1, 0:3].reshape(3 * KC, N))
    for way in range(2):
        with jax.named_scope("far1"):
            gathered_far(1, way)
        r = rows(way, RB)
        res = (acc[r, :] + mm(g[r, gat(1, 3) : gat(1, 4)], w[1, 3])).astype(BF16)
        first = res[:, 0 : N // 2]
        second = res[:, N // 2 : N]
        osw[r, :] = jnp.where(c == 0, second.astype(F32), first.astype(F32)).astype(BF16)
        o = pl.ds(pl.multiple_of(c * H + way * RB, RB), RB)
        rcopy(osw.at[r, :], out.at[o, :], sent, osr.at[0], {"c": other}).start()
        out[o, :] = jnp.where(c == 0, first.astype(F32), second.astype(F32)).astype(BF16)

    few = ((NY - 1) * (Q + 16) + (NY - 1) * Q) // 2 + 8
    KB64 = 16 * D * 2
    weights = 2 * N * (3 * Q + F + 2 * 3 * Q + 3 * Q + 3 * F)
    values = 2 * F * (8 * RB + 2 * 2 * RB + H) + 2 * RB * (N // 2)
    many = 2 * (weights + values)
    for n in range(1, NZ):
        @pl.when(NZ - 1 - z == n)
        def _():
            left(rz.at[0:n], sent_z)
    left(lbuf.at[0:few], sent_s)
    left(tok.at[0 : many // KB64 * 16], sent)
    with jax.named_scope("swap_wait"):
        arrived(out.at[0:H, :], osr.at[0])


def body(NZ, NY, NX, *args):
    (tokens, in_gain, wq, wf, wi, wo, wh, wb, wc, floor, leak, sgain, taps, ggain, ost, ocv) = args
    T, D = tokens.shape
    N = D // NX
    row = lambda a: a.reshape(1, -1)
    V, S = pltpu.VMEM, pltpu.SemaphoreType.DMA
    nc = T // CH
    Q = F // NY
    scratch = [
        V((T, D), BF16), V((D, 2 * F), BF16), V((D, 5 * F), BF16),
        V((1, D), F32), V((D, F), F32), V((3, 1, F), F32), V((3, F), BF16),
        V((T, F), F32), V((2, F, D), BF16),
        V((T, F), F32), V((T, F), F32), V((T, F), BF16), V((T, F), BF16), V((T, F), F32),
        V((nc, F, F), BF16), V((nc, 8, F), F32), V((T, F), BF16), V((T, F), F32), V((T, F), F32),
        V((T + 8, F), F32), V((T, F), F32),
        V((NY, Q + 16, F), BF16), V((NY, Q + 16, F), BF16), V((Q + 16, F), BF16), V((NZ, Q + 16, F), BF16),
        V((NY, Q, F), BF16), V((F, F), BF16), V((8, F), F32), V((2, T, F), BF16),
        V((T // 2, 4 * F * NX), BF16), V((2, NX, 2 * F, N), BF16), V((T // 2, N), F32), V((T // 2, N // 2), BF16),
        S((10,)), S((4,)), S((2, 2, 2)), S((2, 2)), S((2,)), S((1,)), S((2,)), S((2,)), S((2,)), S((1,)), S((3,)),
    ]
    return pl.pallas_call(
        functools.partial(kernel, NZ, NY, NX, T, D),
        name="mixer",
        out_shape=pltpu.VMEM((T, N // 2), BF16),
        in_specs=[pl.BlockSpec(memory_space=pl.ANY)] * 16,
        out_specs=pl.BlockSpec(memory_space=pltpu.VMEM),
        scratch_shapes=scratch,
        compiler_params=pltpu.CompilerParams(
            collective_id=0, has_side_effects=True, vmem_limit_bytes=58 * 1024 * 1024
        ),
    )(
        tokens, row(in_gain), wq, wf, wi, wo, wh, wb, wc, row(floor), leak, row(sgain), taps, row(ggain), ost, ocv
    )


def solution(mesh):
    NZ, NY, NX = 8, 4, 4
    split = Mesh(mesh.devices.reshape(NZ, NY, NX, 2), ("z", "y", "x", "c"))
    sp, tp = ("z", "y"), ("x", "c")
    wide = P(None, tp)
    placed = (
        P(sp, None), P(), wide, wide, wide, wide, wide, wide, wide, P(tp), P(sp, tp), P(), wide, P(), P(tp, None), P(tp, None),
    )
    return jax.shard_map(
        functools.partial(body, NZ, NY, NX), mesh=split, in_specs=placed, out_specs=P(sp, tp), check_vma=False
    )
```

```python
import functools

import jax
import jax.numpy as jnp
from jax import lax
from jax.experimental import pallas as pl
from jax.experimental.pallas import tpu as pltpu
from jax.sharding import Mesh
from jax.sharding import PartitionSpec as P

F = 128
CH = 128
RB = 256
EPS = 1e-6
MESH = pl.DeviceIdType.MESH
F32, BF16 = jnp.float32, jnp.bfloat16
NT = (((1,), (1,)), ((), ()))
TN = (((0,), (0,)), ((), ()))


def mm(a, b):
    return jnp.dot(a, b, preferred_element_type=F32)


def mmg(a, b, dims):
    return lax.dot_general(a, b, dims, preferred_element_type=F32)


LOG_TERMS = (0.9999999971754615, 0.500001179512937, 0.3332539552536287, 0.25193518431296363, 0.17907403058358232, 0.2660849487304504)


def log_part(k):
    p = jnp.full_like(k, LOG_TERMS[-1])
    for term in LOG_TERMS[-2::-1]:
        p = p * k + term
    return p * k


def far_first(n):
    return sorted(range(1, n), key=lambda d: (-min(d, n - d), d))


def silu(v):
    return v * jax.nn.sigmoid(v)


def kernel(
    NZ, NY, NX, T, D,
    tok_h, gain_h, wq_h, wf_h, wi_h, wo_h, wh_h, wb_h, wc_h, floor_h, leak_h, sgain_h, taps_h, ggain_h, ost_h, ocv_h,
    out,
    tok, wfv, wrest, gain, gcol, small, taps, leak, wout,
    rs, fbuf, km, vb, lbuf, sst, lst, qg, ol, gate, cpad, bproj,
    my, ry, mz, rz, mb, pre_s, pre_d, sin, rim, act, g, w, acc, osw,
    ld, xr, ar, rlr, sbr, w1r, w2r, w3r, wfr, osr, sends, here,
):
    z, y, x, c = (lax.axis_index(a) for a in ("z", "y", "x", "c"))
    H = T // 2
    nb, nc = T // RB, T // CH
    N = D // NX
    KC = 2 * F

    def rcopy(src, dst, ss, rsem, dev):
        return pltpu.make_async_remote_copy(
            src_ref=src, dst_ref=dst, send_sem=ss, recv_sem=rsem, device_id=dev, device_id_type=MESH
        )

    def arrived(dst, sem):
        rcopy(dst, dst, sem, sem, {"c": 1 - c}).wait_recv()

    def left(src, sem):
        rcopy(src, src, sem, sem, {"c": 1 - c}).wait_send()

    nxt_y = lax.rem(y + 1, NY)
    nxt_z = lax.rem(z + (y + 1) // NY, NZ)
    prv_y = lax.rem(y + NY - 1, NY)
    prv_z = lax.rem(z + NZ - (NY - y) // NY, NZ)
    nxt = {"z": nxt_z, "y": nxt_y}
    prv = {"z": prv_z, "y": prv_y}
    other = 1 - c
    sent, sent_s, sent_z = sends.at[0], sends.at[1], sends.at[2]

    lds = {}

    def load(name, whole, *pairs):
        sem = ld.at[len(lds)]
        lds[name] = whole, sem
        for src, dst in pairs:
            pltpu.make_async_copy(src, dst, sem).start()

    def need(*names):
        for name in names:
            whole, sem = lds[name]
            pltpu.make_async_copy(whole, whole, sem).wait()

    def rows(i, n):
        return pl.ds(i * n, n)

    def load_rows(i):
        r = rows(i, RB)
        load(f"t{i}", tok.at[r], (tok_h.at[r], tok.at[r]))

    def load_pair(name, ref, left_h, right_h):
        load(name, ref, (left_h, ref.at[:, 0:F]), (right_h, ref.at[:, F : 2 * F]))

    def load_pair(ref, at, left_h, right_h):
        return (left_h, ref.at[:, at : at + F]), (right_h, ref.at[:, at + F : at + 2 * F])

    HALF = pl.ds(T // 2, T // 2)
    load("gain", gain, (gain_h, gain))
    load("t0", tok.at[0:RB], (tok_h.at[0:RB], tok.at[0:RB]))
    load("wfv", wfv, *load_pair(wfv, 0, wf_h, wi_h))
    load("t1", tok.at[RB : 2 * RB], (tok_h.at[RB : 2 * RB], tok.at[RB : 2 * RB]))
    load("small", small, (floor_h, small.at[0]), (sgain_h, small.at[1]), (ggain_h, small.at[2]))
    load("t2", tok.at[HALF], (tok_h.at[HALF], tok.at[HALF]))
    load("leak", leak, (leak_h, leak))
    load("wout", wout, (ocv_h, wout.at[0]), (ost_h, wout.at[1]))

    ahead = z + y == 0
    behind = z + y > 0

    bar = pltpu.get_barrier_semaphore()

    def signal(sem, **to):
        pl.semaphore_signal(sem, inc=1, device_id=to, device_id_type=MESH)

    for d in range(1, NX):
        for e in range(2):
            signal(bar, x=lax.rem(x + d, NX), c=e)
    signal(bar, c=other)
    near = 2 * (NX - 1) + 1
    for d in range(1, NY):
        to_y = lax.rem(y + d, NY)

        @pl.when(z + to_y > 0)
        def _():
            signal(bar, y=to_y)

    for d in range(1, NZ):
        to_z = lax.rem(z + d, NZ)

        @pl.when(to_z + y > 0)
        def _():
            signal(bar, z=to_z)

    @pl.when(nxt_z + nxt_y > 0)
    def _():
        signal(bar, **nxt)

    @pl.when(prv_z + prv_y > 0)
    def _():
        signal(bar, **prv)

    def meet():
        need("wout")

        @pl.when(ahead)
        def _():
            pl.semaphore_wait(bar, near)

        @pl.when(behind)
        def _():
            pl.semaphore_wait(bar, near + (NY - 1) + (NZ - 1) + 2)

        @pl.when(jnp.logical_and(z == 0, y > 0))
        def _():
            signal(here.at[0], y=0)

        @pl.when(jnp.logical_and(z > 0, y == 0))
        def _():
            signal(here.at[1], z=0)

    def turn_gain():
        for k in range(D // F):
            r = rows(k, F)
            gcol[r, :] = jnp.transpose(jnp.broadcast_to(gain[:, k * F : (k + 1) * F], (F, F)))

    def scale(ref):
        for k in range(D // F):
            r = rows(k, F)
            for n in range(ref.shape[1] // F):
                v = ref[r, n * F : (n + 1) * F].astype(F32) * gcol[r, :]
                ref[r, n * F : (n + 1) * F] = v.astype(BF16)

    def norms(i):
        for k in range(RB // 64):
            q = pl.ds(i * RB + k * 64, 64)
            t = tok[q, :]
            t = t * t
            t = t[:, 0 : D // 2] + t[:, D // 2 : D]
            t = (t[:, 0 : D // 4] + t[:, D // 4 : D // 2]).astype(F32)
            ms = jnp.sum(t, axis=-1, keepdims=True) * (1.0 / D)
            rs[q, :] = jnp.broadcast_to(lax.rsqrt(ms + EPS), (64, F))

    def fv(i):
        r = rows(i, T // 2)
        p = mm(tok[r, :], wfv[...])
        s = rs[r, :]
        fbuf[r, :] = p[:, 0:F] * s
        vb[r, :] = (p[:, F : 2 * F] * s).astype(BF16)

    ri = lax.broadcasted_iota(jnp.int32, (CH, CH), 0)
    ci = lax.broadcasted_iota(jnp.int32, (CH, CH), 1)
    causal = ri >= ci
    tri = jnp.where(causal, 1.0, 0.0).astype(BF16)

    def block(i, state, start):
        r = rows(i, CH)
        k = (1.0 - small[0]) * jax.nn.sigmoid(-fbuf[r, :])
        lf = leak[r, :] - log_part(k)
        hi = lf.astype(BF16)
        lo = (lf - hi.astype(F32)).astype(BF16)
        two = mm(tri, jnp.concatenate([hi, lo], axis=1))
        cum = two[:, 0:F] + two[:, F : 2 * F]
        total = cum[CH - 1 : CH, :]
        mid = cum[CH // 2 - 1 : CH // 2, :]
        lbuf[r, :] = cum
        lst[i] = jnp.broadcast_to(start, (8, F))
        kmid = k * jnp.exp(mid - cum)
        km[r, :] = kmid.astype(BF16)
        kd = (kmid * jnp.exp(total - mid)).astype(BF16)
        sst[i] = state.astype(BF16)
        state = state * jnp.exp(total) + mmg(vb[r, :], kd, TN)
        return state, start + total

    state, start = jnp.zeros((F, F), F32), jnp.zeros((1, F), F32)
    Q = F // NY
    wpart = pl.ds(pl.multiple_of(y * Q, Q), Q)
    wmine = pl.ds(pl.multiple_of(c * F + y * Q, Q), Q)
    wcore = pl.ds(pl.multiple_of(c * F, F), F)

    def wspread(kind):
        part_w = w.at[kind, 1:NX, wmine, :]
        for d in (1, NY - 1):
            rcopy(part_w, part_w, sent, w2r.at[kind], {"y": lax.rem(y + d, NY)}).start()

    def wrelay(kind):
        arrived(w.at[kind, 1:NX, 0 : 2 * Q, :], w2r.at[kind])
        for d in (1, NY - 1):
            source = lax.rem(y + NY - d, NY)
            at = c * F + source * Q + (0 if d == 1 else Q // 2)
            part_w = w.at[kind, 1:NX, pl.ds(pl.multiple_of(at, Q // 2), Q // 2), :]
            rcopy(part_w, part_w, sent, w3r.at[kind], {"y": lax.rem(y + d, NY)}).start()

    def wforward(kind):
        arrived(w.at[kind, 1:NX, 0:Q, :], w3r.at[kind])
        part_w = w.at[kind, 1:NX, wcore, :]
        rcopy(part_w, part_w, sent, wfr.at[kind], {"c": other}).start()
    def greet():
        with jax.named_scope("barrier_wait"):
            meet()
        for kind in range(2):
            for d, slot in ((2, 3), (1, 1), (NX - 1, 2)):
                to = lax.rem(x + d, NX)
                rcopy(
                    wout.at[kind, wpart, pl.ds(pl.multiple_of(to * N, N), N)],
                    w.at[kind, slot, wmine, :], sent, w1r.at[kind], {"x": to},
                ).start()
            own = wout.at[kind, :, pl.ds(pl.multiple_of(x * N, N), N)]
            rcopy(own, w.at[kind, 0, wcore, :], sent, wfr.at[kind], {"c": other}).start()

    r16 = lax.broadcasted_iota(jnp.int32, (16, F), 0)

    def decay_rows(dec):
        top = dec.astype(BF16)
        low = (dec - top.astype(F32)).astype(BF16)
        return jnp.where(r16 == 0, top.astype(F32), low.astype(F32)).astype(BF16)

    def part(ref, k):
        dec = ref[k, Q : Q + 16, :].astype(F32)
        return ref[k, 0:Q, :].astype(F32), dec[0:1, :] + dec[1:2, :]

    def first_step():
        for d in far_first(NY):
            to = lax.rem(y + d, NY)
            rcopy(my.at[to], ry.at[y], sent_s, xr.at[0], {"y": to}).start()

    def second_step():
        with jax.named_scope("s1_wait"):
            arrived(ry.at[0 : NY - 1], xr.at[0])
        ps, pd = jnp.zeros((Q, F), F32), jnp.ones((1, F), F32)
        for k in range(NY):
            pre_s[k] = ps
            pre_d[k] = jnp.broadcast_to(pd, (8, F))
            s, dec = part(ry, k)
            ps, pd = ps * dec + s, pd * dec
        @pl.when(ahead)
        def _():
            pl.semaphore_wait(here.at[1], NZ - 1)

        mz[0:Q, :] = ps.astype(BF16)
        mz[Q : Q + 16, :] = decay_rows(pd)
        for d in far_first(NZ):
            @pl.when(z + d < NZ)
            def _():
                rcopy(mz, rz.at[z], sent_z, xr.at[1], {"z": lax.rem(z + d, NZ)}).start()

    def third_step():
        with jax.named_scope("s2_wait"):
            for n in range(1, NZ):
                @pl.when(z == n)
                def _():
                    arrived(rz.at[0:n], xr.at[1])
        before = jnp.zeros((Q, F), F32)
        for k in range(NZ - 1):
            s, dec = part(rz, k)
            before = jnp.where(k < z, before * dec + s, before)
        for k in range(NY):
            mb[k] = (before * pre_d[k][0:1, :] + pre_s[k]).astype(BF16)
        mine = pl.ds(pl.multiple_of(y * Q, Q), Q)
        sin[mine, :] = mb[y]
        for d in far_first(NY):
            to = lax.rem(y + d, NY)
            rcopy(mb.at[to], sin.at[mine, :], sent_s, xr.at[2], {"y": to}).start()

    def third_arrived():
        with jax.named_scope("s3_wait"):
            arrived(sin.at[0 : F - Q, :], xr.at[2])

    def hcb(i):
        r = rows(i, RB)
        s = rs[r, :]
        p = mm(tok[r, :], wrest[:, 0 : 2 * F])
        cpad[pl.ds(8 + i * RB, RB), :] = ((p[:, 0:F] * s) * (p[:, F : 2 * F] * s)).astype(BF16).astype(F32)
        bproj[r, :] = mm(tok[r, :], wrest[:, 2 * F : 3 * F]) * s

    def send_rim():
        rcopy(cpad.at[pl.ds(T, 8), :], rim, sent_s, xr.at[3], nxt).start()

    def conv(i):
        tf = taps[...].astype(F32)
        r = rows(i, RB)
        total = tf[0:1, :] * cpad[pl.ds(6 + i * RB, RB), :]
        total = total + tf[1:2, :] * cpad[pl.ds(7 + i * RB, RB), :]
        total = total + tf[2:3, :] * cpad[pl.ds(8 + i * RB, RB), :]
        v = bproj[r, :] * total
        ms = jnp.mean(v * v, axis=-1, keepdims=True)
        act[0, r, :] = (v * lax.rsqrt(ms + EPS) * small[2]).astype(BF16)

    def qo(i):
        r = rows(i, RB)
        s = rs[r, :]
        p = mm(tok[r, :], wrest[:, 3 * F : 5 * F])
        fbuf[r, :] = silu(p[:, 0:F] * s)
        gate[r, :] = silu(p[:, F : 2 * F] * s) * small[1]

    def reads(i):
        r = rows(i, CH)
        cum = lbuf[r, :]
        q = fbuf[r, :]
        mid = cum[CH // 2 - 1 : CH // 2, :]
        qmid = q * jnp.exp(cum - mid)
        qm = qmid.astype(BF16)
        ql = (qmid * jnp.exp(mid)).astype(BF16)
        qg[r, :] = (qmid * jnp.exp(mid + lst[i][0:1, :])).astype(BF16)
        scores = jnp.where(causal, mmg(qm, km[r, :], NT), 0.0).astype(BF16)
        ol[r, :] = mm(scores, vb[r, :]) + mmg(ql, sst[i], NT)

    def gat(kind, slot):
        return kind * NX * KC + slot * KC

    def send(kind, way, part_k, e):
        to = lax.rem(x + (1 if way == 0 else NX - 1), NX)
        rcopy(
            act.at[kind, pl.ds(e * H + part_k * RB, RB), :],
            g.at[pl.ds(part_k * RB, RB), pl.ds(pl.multiple_of(gat(kind, 1 + way) + c * F, F), F)],
            sent, ar.at[kind, way, part_k], {"x": to, "c": e},
        ).start()

    def keep(kind):
        place = g.at[:, pl.ds(pl.multiple_of(gat(kind, 0) + c * F, F), F)]
        rcopy(
            act.at[kind, pl.ds(pl.multiple_of(other * H, H), H), :], place, sent, sbr.at[kind], {"c": other}
        ).start()
        place[...] = act[kind, pl.ds(pl.multiple_of(c * H, H), H), :]

    def gblock(kind, slot, part_k):
        return g.at[pl.ds(part_k * RB, RB), pl.ds(gat(kind, slot), KC)]

    def relayed(kind, way):
        part_k = way
        to = lax.rem(x + (1 if way == 0 else NX - 1), NX)
        arrived(gblock(kind, 1 + way, part_k), ar.at[kind, way, part_k])
        rcopy(
            g.at[pl.ds(part_k * RB, RB), pl.ds(gat(kind, 1 + way), KC)],
            g.at[pl.ds(part_k * RB, RB), pl.ds(gat(kind, 3), KC)],
            sent, rlr.at[kind, way], {"x": to},
        ).start()

    def gathered_near(kind):
        for way in range(2):
            part_k = 1 - way
            arrived(gblock(kind, 1 + way, part_k), ar.at[kind, way, part_k])
        arrived(g.at[:, pl.ds(0, F)], sbr.at[kind])

    def gathered_far(kind, way):
        arrived(g.at[pl.ds(way * RB, RB), pl.ds(gat(kind, 3), KC)], rlr.at[kind, way])

    def send_conv():
        send(0, 1, 1, 0)
        send(0, 0, 0, 1)
        send(0, 1, 1, 1)
        send(0, 0, 1, 0)

    def finish(i, carried):
        r = rows(i, RB)
        v = ol[r, :]
        if carried:
            v = v + mmg(qg[r, :], sin[...], NT)
        ms = jnp.mean(v * v, axis=-1, keepdims=True)
        act[1, r, :] = (v * lax.rsqrt(ms + EPS) * gate[r, :]).astype(BF16)

    def finish_all(carried):
        with jax.named_scope("finish"):
            finish(0, carried)
            finish(2, carried)
            send(1, 0, 0, 0)
            send(1, 0, 0, 1)
            finish(1, carried)
            finish(3, carried)
            for e in range(2):
                send(1, 1, 1, e)
            for e in range(2):
                send(1, 0, 1, e)
            for e in range(2):
                send(1, 1, 0, e)
            keep(1)

    def w_near(kind):
        with jax.named_scope("w_near"):
            arrived(w.at[kind, 1:NX, 0:Q, :], w1r.at[kind])
            wspread(kind)

    with jax.named_scope("head"):
        need("gain")
        turn_gain()
        need("t0")
        norms(0)
        need("wfv")
        scale(wfv)
        need("t1")
        norms(1)
    per = RB // CH
    with jax.named_scope("first"):
        fv(0)
    need("t2", "small", "leak")
    load("wrest", wrest, *load_pair(wrest, 0, wh_h, wc_h), (wb_h, wrest.at[:, 2 * F : 3 * F]), *load_pair(wrest, 3 * F, wq_h, wo_h))
    load("taps", taps, (taps_h, taps))
    with jax.named_scope("first"):
        norms(2)
        norms(3)
        fv(1)
        for j in range(nc // 2):
            state, start = block(j, state, start)
    greet()
    with jax.named_scope("last_blocks"):
        for j in range(nc // 2, nc):
            state, start = block(j, state, start)
    drow = decay_rows(jnp.exp(start))
    for q in range(NY):
        my[q, 0:Q, :] = state[q * Q : (q + 1) * Q, :].astype(BF16)
        my[q, Q : Q + 16, :] = drow
    ry[y] = my[y]
    pl.when(behind)(first_step)

    with jax.named_scope("w_wait"):
        need("wrest", "taps")
    scale(wrest.at[:, 0 : 3 * F])
    hcb(nb - 1)
    pl.when(behind)(send_rim)
    with jax.named_scope("hcb"):
        for i in range(nb - 2, -1, -1):
            hcb(i)
    with jax.named_scope("conv"):
        for i in range(nb - 1, 0, -1):
            conv(i)

    send_conv()

    @pl.when(behind)
    def _():
        w_near(0)

    with jax.named_scope("qo"):
        scale(wrest.at[:, 3 * F : 5 * F])
        qo(0)
        qo(1)
        for j in range(per):
            reads(j)
        for kind in range(2):
            w[kind, 0, wcore, :] = wout[kind, :, pl.ds(pl.multiple_of(x * N, N), N)]

    pl.when(behind)(second_step)

    with jax.named_scope("qo"):
        for i in range(2, nb):
            qo(i)
            for j in range((i - 1) * per, i * per):
                reads(j)
        for j in range((nb - 1) * per, nc):
            reads(j)

    @pl.when(behind)
    def _():
        with jax.named_scope("rim_wait"):
            arrived(rim, xr.at[3])
        cpad[0:8, :] = rim[...]

    @pl.when(ahead)
    def _():
        cpad[0:8, :] = jnp.zeros((8, F), F32)

    with jax.named_scope("spread0"):
        conv(0)
        send(0, 0, 0, 0)
        send(0, 1, 0, 0)
        send(0, 0, 1, 1)
        send(0, 1, 0, 1)
        keep(0)

    @pl.when(ahead)
    def _():
        finish_all(False)
        with jax.named_scope("here"):
            pl.semaphore_wait(here.at[0], NY - 1)
        first_step()
        send_rim()
        second_step()
        w_near(0)

    third_step()
    with jax.named_scope("wrelay0"):
        w_near(1)
        wrelay(0)
    with jax.named_scope("relay0"):
        relayed(0, 0)
        relayed(0, 1)

    @pl.when(behind)
    def _():
        third_arrived()
        finish_all(True)

    with jax.named_scope("wfr_near0"):
        wforward(0)
        wrelay(1)
        gathered_near(0)
        arrived(w.at[0, :, 0:F, :], wfr.at[0])
    for way in range(2):
        with jax.named_scope("far0"):
            gathered_far(0, way)
        r = rows(way, RB)
        acc[r, :] = mm(g[r, 0 : NX * KC], w[0].reshape(NX * KC, N))
    with jax.named_scope("relay1"):
        relayed(1, 0)
        relayed(1, 1)
    with jax.named_scope("wforward1"):
        wforward(1)
    with jax.named_scope("near1"):
        gathered_near(1)
        arrived(w.at[1, :, 0:F, :], wfr.at[1])
    for way in range(2):
        r = rows(way, RB)
        acc[r, :] = acc[r, :] + mm(g[r, gat(1, 0) : gat(1, 3)], w[1, 0:3].reshape(3 * KC, N))
    for way in range(2):
        with jax.named_scope("far1"):
            gathered_far(1, way)
        r = rows(way, RB)
        res = (acc[r, :] + mm(g[r, gat(1, 3) : gat(1, 4)], w[1, 3])).astype(BF16)
        first = res[:, 0 : N // 2]
        second = res[:, N // 2 : N]
        osw[r, :] = jnp.where(c == 0, second.astype(F32), first.astype(F32)).astype(BF16)
        o = pl.ds(pl.multiple_of(c * H + way * RB, RB), RB)
        rcopy(osw.at[r, :], out.at[o, :], sent, osr.at[0], {"c": other}).start()
        out[o, :] = jnp.where(c == 0, first.astype(F32), second.astype(F32)).astype(BF16)

    @pl.when(ahead)
    def _():
        arrived(rim, xr.at[3])
        third_arrived()

    few = ((NY - 1) * (Q + 16) + (NY - 1) * Q) // 2 + 8
    KB64 = 16 * D * 2
    weights = 2 * N * (3 * Q + F + 2 * 3 * Q + 3 * Q + 3 * F)
    values = 2 * F * (8 * RB + 2 * 2 * RB + H) + 2 * RB * (N // 2)
    many = 2 * (weights + values)
    for n in range(1, NZ):
        @pl.when(NZ - 1 - z == n)
        def _():
            left(rz.at[0:n], sent_z)
    left(lbuf.at[0:few], sent_s)
    left(tok.at[0 : many // KB64 * 16], sent)
    with jax.named_scope("swap_wait"):
        arrived(out.at[0:H, :], osr.at[0])


def body(NZ, NY, NX, *args):
    (tokens, in_gain, wq, wf, wi, wo, wh, wb, wc, floor, leak, sgain, taps, ggain, ost, ocv) = args
    T, D = tokens.shape
    N = D // NX
    row = lambda a: a.reshape(1, -1)
    V, S = pltpu.VMEM, pltpu.SemaphoreType.DMA
    nc = T // CH
    Q = F // NY
    scratch = [
        V((T, D), BF16), V((D, 2 * F), BF16), V((D, 5 * F), BF16),
        V((1, D), F32), V((D, F), F32), V((3, 1, F), F32), V((3, F), BF16),
        V((T, F), F32), V((2, F, D), BF16),
        V((T, F), F32), V((T, F), F32), V((T, F), BF16), V((T, F), BF16), V((T, F), F32),
        V((nc, F, F), BF16), V((nc, 8, F), F32), V((T, F), BF16), V((T, F), F32), V((T, F), F32),
        V((T + 8, F), F32), V((T, F), F32),
        V((NY, Q + 16, F), BF16), V((NY, Q + 16, F), BF16), V((Q + 16, F), BF16), V((NZ, Q + 16, F), BF16),
        V((NY, Q, F), BF16), V((NY, Q, F), F32), V((NY, 8, F), F32), V((F, F), BF16), V((8, F), F32), V((2, T, F), BF16),
        V((T // 2, 4 * F * NX), BF16), V((2, NX, 2 * F, N), BF16), V((T // 2, N), F32), V((T // 2, N // 2), BF16),
        S((10,)), S((4,)), S((2, 2, 2)), S((2, 2)), S((2,)), S((2,)), S((2,)), S((2,)), S((2,)), S((1,)), S((3,)), pltpu.SemaphoreType.REGULAR((2,)),
    ]
    return pl.pallas_call(
        functools.partial(kernel, NZ, NY, NX, T, D),
        name="mixer",
        out_shape=pltpu.VMEM((T, N // 2), BF16),
        in_specs=[pl.BlockSpec(memory_space=pl.ANY)] * 16,
        out_specs=pl.BlockSpec(memory_space=pltpu.VMEM),
        scratch_shapes=scratch,
        compiler_params=pltpu.CompilerParams(
            collective_id=0, has_side_effects=True, vmem_limit_bytes=58 * 1024 * 1024
        ),
    )(
        tokens, row(in_gain), wq, wf, wi, wo, wh, wb, wc, row(floor), leak, row(sgain), taps, row(ggain), ost, ocv
    )


def solution(mesh):
    NZ, NY, NX = 8, 4, 4
    split = Mesh(mesh.devices.reshape(NZ, NY, NX, 2), ("z", "y", "x", "c"))
    sp, tp = ("z", "y"), ("x", "c")
    wide = P(None, tp)
    placed = (
        P(sp, None), P(), wide, wide, wide, wide, wide, wide, wide, P(tp), P(sp, tp), P(), wide, P(), P(tp, None), P(tp, None),
    )
    return jax.shard_map(
        functools.partial(body, NZ, NY, NX), mesh=split, in_specs=placed, out_specs=P(sp, tp), check_vma=False
    )
```
